128 devices in a mesh: sp: 16 (over z, x), dp: 8 (over y, core).
Axes of the slice: x: 4, y: 4, z: 4, core: 2. Of those that a mesh axis runs over, the one named last changes fastest.
Arguments:
- hidden_in: bfloat16 [8, 2048, 2048], P('dp', 'sp'), may hold values from -6 to 6
- mix_cotangent: bfloat16 [8, 2048, 4096], P('dp', 'sp'), may hold values from -0.119628906 to 0.119628906
- query_weight: bfloat16 [2048, 4096], P('dp', 'sp'), may hold values from -0.125 to 0.125
- key_weight: bfloat16 [2048, 4096], P('dp', 'sp'), may hold values from -0.125 to 0.125
- value_weight: bfloat16 [2048, 4096], P('dp', 'sp'), may hold values from -0.125 to 0.125
- decay_log: float32 [16], P('sp'), may hold values from -0.034 to -0.000146484375, as said below
Outputs:
- grad_hidden: bfloat16 [8, 2048, 2048], P('dp', 'sp')
- grad_query: float32 [2048, 4096], P('dp', 'sp')
- grad_key: float32 [2048, 4096], P('dp', 'sp')
- grad_value: float32 [2048, 4096], P('dp', 'sp')
The draws below stay inside these ranges and needn't reach their ends.
Inputs may be any that keep to these rules, and one draw needn't show every extreme that they name: Each head's decay_log is negative.
All inputs are finite; a program needn't handle non-finite values.
Results may differ from the reference program's by a relative error of at most 0.015.
Values may be sent and summed in bfloat16 or wider, within the bound.
No kernel may reach another device: no remote copies, remote signals or barrier semaphores. Data moves between devices by JAX's collectives and lax.ppermute only.
A program may use at most 64 MiB of HBM per device.

```python
import jax
import jax.numpy as jnp
from jax import lax

D = 2048
HEADS = 16
BLOCK = 128
WIDTH = 4096
SEQ_LEN = 2048
SEQS = 8
N_SP = 16


def draw_decay_log(key, part):
    key_fast = jax.random.fold_in(key, 11)
    key_quick = jax.random.fold_in(key, 12)
    key_slow = jax.random.fold_in(key, 13)
    fast = jax.random.bernoulli(key_fast, 0.5, (HEADS,))
    quick_rate = jax.random.uniform(key_quick, (HEADS,), jnp.float32, 0.01, 0.034)
    slow_rate = jax.random.uniform(key_slow, (HEADS,), jnp.float32, 0.3, 2.0) / SEQ_LEN
    return -jnp.where(fast, quick_rate, slow_rate).astype(jnp.float32)


def block_levels(own_key, extent, cuts, smallest, largest):
    gain = 1.0
    for position, parts in cuts:
        heights = jax.random.uniform(jax.random.fold_in(jax.random.fold_in(own_key, 6), position), (parts,), jnp.float32, smallest / len(cuts), largest / len(cuts))
        gain = gain * jnp.repeat(jnp.exp(heights), extent[position] // parts).reshape((-1,) + (1,) * (len(extent) - 1 - position))
    return gain


def noise(rng, extent, scale, reach, split=(), kind=jnp.bfloat16):
    array = scale * jax.random.normal(rng, extent, jnp.float32)
    if split:
        array = array * block_levels(rng, extent, split, -0.22, 0.18)
    return jnp.clip(array, -reach, reach).astype(kind)


def setup_inputs(seed: int = 0) -> dict:
    seeds = jax.random.split(jax.random.key(seed), 7)
    return {
        "hidden_in": noise(seeds[0], (SEQS, SEQ_LEN, D), 1.0, 6.0, ((0, 8), (1, 16))),
        "mix_cotangent": noise(seeds[1], (SEQS, SEQ_LEN, WIDTH), 0.02, 0.119628906, ((0, 8), (1, 16))),
        "query_weight": noise(seeds[2], (D, WIDTH), D ** -0.5, 0.125, ((0, 8), (1, 16))),
        "key_weight": noise(seeds[3], (D, WIDTH), D ** -0.5, 0.125, ((0, 8), (1, 16))),
        "value_weight": noise(seeds[4], (D, WIDTH), D ** -0.5, 0.125, ((0, 8), (1, 16))),
        "decay_log": draw_decay_log(jax.random.fold_in(seeds[6], 71), 0),
    }


def head_grads(queries, key_rows, values, cotangent, log_rate):
    length = queries.shape[0]
    head_dim = queries.shape[1]
    blocks = length // BLOCK
    scale = head_dim ** -0.5
    keys_scaled = (key_rows.astype(jnp.float32) * scale).astype(jnp.bfloat16)
    offsets = jnp.arange(BLOCK, dtype=jnp.float32)
    spread = offsets[:, None] - offsets[None, :]
    inner_decay = jnp.where(spread >= 0, jnp.exp(log_rate * jnp.maximum(spread, 0.0)), 0.0)
    query_decay = jnp.exp(log_rate * (offsets + 1.0))
    key_decay = jnp.exp(log_rate * (BLOCK - 1.0 - offsets))
    block_decay = jnp.exp(log_rate * BLOCK)

    def split_blocks(series):
        return series.reshape(blocks, BLOCK, series.shape[-1])

    def forward(carried, inputs):
        query_block, key_block, value_block, grad_block = inputs
        mixed = (jnp.dot(grad_block, value_block.T, preferred_element_type=jnp.float32) * inner_decay).astype(jnp.bfloat16)
        within = jnp.dot(mixed, key_block, preferred_element_type=jnp.float32)
        across = jnp.dot(grad_block, carried.astype(jnp.bfloat16).T, preferred_element_type=jnp.float32) * query_decay[:, None]
        weighted = (key_block.astype(jnp.float32) * key_decay[:, None]).astype(jnp.bfloat16)
        updated = carried * block_decay + jnp.dot(weighted.T, value_block, preferred_element_type=jnp.float32)
        return updated, (within + across, mixed)

    def backward(carried, inputs):
        query_block, key_block, value_block, grad_block, mixed = inputs
        scores = (jnp.dot(query_block, key_block.T, preferred_element_type=jnp.float32) * inner_decay).astype(jnp.bfloat16)
        state_bf = carried.astype(jnp.bfloat16)
        grad_v = jnp.dot(scores.T, grad_block, preferred_element_type=jnp.float32) + jnp.dot(key_block, state_bf, preferred_element_type=jnp.float32) * key_decay[:, None]
        grad_k = (jnp.dot(mixed.T, query_block, preferred_element_type=jnp.float32) + jnp.dot(value_block, state_bf.T, preferred_element_type=jnp.float32) * key_decay[:, None]) * scale
        weighted = (query_block.astype(jnp.float32) * query_decay[:, None]).astype(jnp.bfloat16)
        updated = carried * block_decay + jnp.dot(weighted.T, grad_block, preferred_element_type=jnp.float32)
        return updated, (grad_k, grad_v)

    inputs = (split_blocks(queries), split_blocks(keys_scaled), split_blocks(values), split_blocks(cotangent))
    initial = jnp.zeros((head_dim, values.shape[-1]), jnp.float32)
    final_state, (grad_q, mixed_all) = lax.scan(forward, initial, inputs)
    final_back, (grad_k, grad_v) = lax.scan(backward, initial, inputs + (mixed_all,), reverse=True)
    return grad_q.reshape(length, -1), grad_k.reshape(length, -1), grad_v.reshape(length, -1)


def group_grads(log_rates, queries, key_rows, values, cotangent):
    length = queries.shape[0]
    head_count = log_rates.shape[0]

    def by_head(series):
        return series.reshape(length, head_count, -1).transpose(1, 0, 2)

    def to_rows(series):
        return series.transpose(1, 0, 2).reshape(length, -1)

    grad_q, grad_k, grad_v = jax.vmap(head_grads)(by_head(queries), by_head(key_rows), by_head(values), by_head(cotangent), log_rates)
    return jnp.concatenate((to_rows(grad_q), to_rows(grad_k), to_rows(grad_v)), axis=1).astype(jnp.bfloat16)


def reference(hidden_in, mix_cotangent, query_weight, key_weight, value_weight, decay_log):
    weights = jnp.concatenate((query_weight, key_weight, value_weight), axis=1)
    all_width = query_weight.shape[1]
    model_width = query_weight.shape[0]

    def one_sequence(seq_pair):
        seq_rows, seq_cotangent = seq_pair
        projected = jnp.dot(seq_rows, weights, preferred_element_type=jnp.float32).astype(jnp.bfloat16)
        gradients = group_grads(decay_log, projected[:, :all_width], projected[:, all_width:2 * all_width], projected[:, 2 * all_width:], seq_cotangent)
        length = seq_rows.shape[0]
        split_grads = gradients.reshape(length, 3, N_SP, -1).astype(jnp.float32)
        split_weights = weights.reshape(model_width, 3, N_SP, -1).astype(jnp.float32)
        partials = jnp.einsum('ltgc,dtgc->gld', split_grads, split_weights)
        rounded = lax.optimization_barrier(partials.astype(jnp.bfloat16)).astype(jnp.float32)
        return jnp.sum(rounded, axis=0).astype(jnp.bfloat16), gradients

    grad_hidden, all_grads = lax.map(one_sequence, (hidden_in, mix_cotangent))
    flat_rows = hidden_in.reshape(-1, model_width)
    flat_grads = all_grads.reshape(-1, 3 * all_width)
    summed = lax.dot_general(flat_rows, flat_grads, (((0,), (0,)), ((), ())), preferred_element_type=jnp.float32) / SEQS
    return grad_hidden, summed[:, :all_width], summed[:, all_width:2 * all_width], summed[:, 2 * all_width:]
```

```python
import jax
import jax.numpy as jnp
from jax import lax
from jax.experimental import pallas as pl
from jax.experimental.pallas import tpu as pltpu
from jax.sharding import PartitionSpec as P


STEP = 256


def dot(a, b, dims):
    return lax.dot_general(a, b, (dims, ((), ())), preferred_element_type=jnp.float32)


def retention_kernel(rate_ref, proj_ref, cot_ref, out_ref, inner_ref, qdec_ref, kdec_ref, fwd_ref, back_ref):
    rate = rate_ref[0]
    dim = cot_ref.shape[1]
    steps = cot_ref.shape[0] // STEP
    scale = dim ** (-0.5)
    row = lax.broadcasted_iota(jnp.int32, (STEP, STEP), 0).astype(jnp.float32)
    col = lax.broadcasted_iota(jnp.int32, (STEP, STEP), 1).astype(jnp.float32)
    spread = row - col
    inner_ref[...] = jnp.where(spread >= 0, jnp.exp(rate * jnp.maximum(spread, 0.0)), 0.0)
    at = lax.broadcasted_iota(jnp.int32, (STEP, dim), 0).astype(jnp.float32)
    qdec_ref[...] = jnp.exp(rate * (at + 1.0))
    kdec_ref[...] = jnp.exp(rate * (STEP - 1.0 - at))
    carry = jnp.exp(jnp.full((dim, dim), STEP * rate, jnp.float32))
    fwd_ref[...] = jnp.zeros_like(fwd_ref)
    back_ref[...] = jnp.zeros_like(back_ref)

    def load(index):
        rows = pl.ds(pl.multiple_of(index * STEP, STEP), STEP)
        queries = proj_ref[rows, 0:dim]
        keys = proj_ref[rows, dim : 2 * dim] * jnp.bfloat16(scale)
        values = proj_ref[rows, 2 * dim : 3 * dim]
        return rows, queries, keys, values, cot_ref[rows, :]

    def step(index, unused):
        rows, queries, keys, values, cot = load(index)
        mixed = (dot(cot, values, ((1,), (1,))) * inner_ref[...]).astype(jnp.bfloat16)
        state = fwd_ref[...]
        grad_q = dot(mixed, keys, ((1,), (0,))) + dot(cot, state.astype(jnp.bfloat16), ((1,), (0,))) * qdec_ref[...]
        keys_w = (keys.astype(jnp.float32) * kdec_ref[...]).astype(jnp.bfloat16)
        fwd_ref[...] = state * carry + dot(values, keys_w, ((0,), (0,)))
        out_ref[rows, 0:dim] = grad_q.astype(jnp.bfloat16)

        rows, queries, keys, values, cot = load(steps - 1 - index)
        mixed = (dot(cot, values, ((1,), (1,))) * inner_ref[...]).astype(jnp.bfloat16)
        scores = (dot(queries, keys, ((1,), (1,))) * inner_ref[...]).astype(jnp.bfloat16)
        state = back_ref[...]
        state_bf = state.astype(jnp.bfloat16)
        grad_v = dot(scores, cot, ((0,), (0,))) + dot(keys, state_bf, ((1,), (0,))) * kdec_ref[...]
        grad_k = dot(mixed, queries, ((0,), (0,))) + dot(values, state_bf, ((1,), (1,))) * kdec_ref[...]
        queries_w = (queries.astype(jnp.float32) * qdec_ref[...]).astype(jnp.bfloat16)
        back_ref[...] = state * carry + dot(queries_w, cot, ((0,), (0,)))
        out_ref[rows, dim : 2 * dim] = (grad_k * scale).astype(jnp.bfloat16)
        out_ref[rows, 2 * dim : 3 * dim] = grad_v.astype(jnp.bfloat16)
        return unused

    lax.fori_loop(0, steps, step, 0)


def retention(rate, projected, cotangent):
    length, dim = cotangent.shape
    square = pltpu.VMEM((STEP, STEP), jnp.float32)
    wide = pltpu.VMEM((STEP, dim), jnp.float32)
    state = pltpu.VMEM((dim, dim), jnp.float32)
    return pl.pallas_call(
        retention_kernel,
        out_shape=jax.ShapeDtypeStruct((length, 3 * dim), jnp.bfloat16),
        in_specs=[
            pl.BlockSpec(memory_space=pltpu.SMEM),
            pl.BlockSpec(memory_space=pltpu.VMEM),
            pl.BlockSpec(memory_space=pltpu.VMEM),
        ],
        out_specs=pl.BlockSpec(memory_space=pltpu.VMEM),
        scratch_shapes=[square, wide, wide, state, state],
        name="retention",
    )(rate, projected, cotangent)


def along_y(array, shift, swap):
    pairs = [
        (y * 2 + c, ((y + shift) % 4) * 2 + (c + swap) % 2) for y in range(4) for c in range(2)
    ]
    return lax.ppermute(array, "dp", pairs)


def all_weight_rows(own):
    index = lax.axis_index("dp")
    y, core = index // 2, index % 2
    before = along_y(own, 1, 0)
    after = along_y(own, -1, 0)
    far = along_y(own, 2, 0)
    mine = jnp.stack((own, after, far, before) * 2)
    mine = lax.dynamic_slice_in_dim(mine, (4 - y) % 4, 4, 0)
    other = along_y(mine, 0, 1)
    first = core == 0
    rows = jnp.stack((jnp.where(first, mine, other), jnp.where(first, other, mine)), axis=1)
    return rows.reshape(-1, own.shape[1])


def body(hidden_in, mix_cotangent, query_weight, key_weight, value_weight, decay_log):
    columns = query_weight.shape[1]
    all_rows = lax.all_gather(hidden_in[0], "sp", axis=0, tiled=True)
    weights = all_weight_rows(jnp.concatenate((query_weight, key_weight, value_weight), axis=1))
    cotangent = lax.all_to_all(mix_cotangent[0], "sp", split_axis=1, concat_axis=0, tiled=True)
    projected = jnp.dot(all_rows, weights, preferred_element_type=jnp.float32).astype(jnp.bfloat16)
    gradients = retention(decay_log, projected, cotangent)
    input_sum = lax.psum_scatter(
        dot(gradients, weights, ((1,), (1,))).astype(jnp.bfloat16),
        "sp",
        scatter_dimension=0,
        tiled=True,
    )
    partial = dot(all_rows, gradients, ((0,), (0,))).astype(jnp.bfloat16)
    parts = lax.axis_size("dp")
    pieces = partial.reshape(parts, -1, 3 * columns)
    arrived = lax.all_to_all(pieces, "dp", split_axis=0, concat_axis=0, tiled=True)
    summed = arrived.astype(jnp.float32).sum(axis=0) / parts
    return (
        input_sum[None],
        summed[:, :columns],
        summed[:, columns : 2 * columns],
        summed[:, 2 * columns :],
    )


def solution(mesh):
    placed = (
        P("dp", "sp", None),
        P("dp", "sp", None),
        P("dp", "sp"),
        P("dp", "sp"),
        P("dp", "sp"),
        P("sp"),
    )
    return jax.shard_map(
        body,
        mesh=mesh,
        in_specs=placed,
        out_specs=(P("dp", "sp", None), P("dp", "sp"), P("dp", "sp"), P("dp", "sp")),
        check_vma=False,
    )
```

```python
import jax
import jax.numpy as jnp
from jax import lax
from jax.experimental import pallas as pl
from jax.experimental.pallas import tpu as pltpu
from jax.sharding import PartitionSpec as P


STEP = 256
UNROLL = 2
HALF = 64
SIDE = 4
GROUP = 2 * SIDE * HALF


def dot(a, b, dims):
    return lax.dot_general(a, b, (dims, ((), ())), preferred_element_type=jnp.float32)


def moved(array, axis, step):
    pairs = []
    for z in range(SIDE):
        for x in range(SIDE):
            to = ((z + step) % SIDE, x) if axis == "z" else (z, (x + step) % SIDE)
            pairs.append((z * SIDE + x, to[0] * SIDE + to[1]))
    return lax.ppermute(array, "sp", pairs)


def along_y(array, shift, swap):
    pairs = [
        (y * 2 + c, ((y + shift) % SIDE) * 2 + (c + swap) % 2) for y in range(SIDE) for c in range(2)
    ]
    return lax.ppermute(array, "dp", pairs)


def gathered(rows, first, second):
    after = moved(rows, first, -1)
    before = moved(rows, first, 1)
    far = moved(rows, first, 2)
    low = jnp.concatenate((rows, after))
    high = jnp.concatenate((far, before))
    low_before = moved(low, second, 1)
    high_after = moved(high, second, -1)
    low_after = moved(low, second, -1)
    high_before = moved(high, second, 1)
    low_far = moved(low_before, second, 1)
    high_far = moved(high_after, second, -1)
    return ((low, high), (low_after, high_after), (low_far, high_far), (low_before, high_before))


def reduced(own, after, far, before, first, second):
    far = moved(far, second, 2)
    after = moved(after, second, 1)
    before = moved(before, second, -1)
    kept, one, two, three = collected(own, after, far, before)
    one = moved(one, first, 1)
    three = moved(three, first, -1)
    two = moved(two, first, 2)
    wide = jnp.float32
    return kept.astype(wide) + one.astype(wide) + three.astype(wide) + two.astype(wide)


def weight_sum(given, kept):
    wide = jnp.float32
    pair = kept.astype(wide) + along_y(given, 0, 1).astype(wide)
    total = pair[0]
    for shift in (1, -1, 2):
        total += along_y(pair[shift % SIDE].astype(jnp.bfloat16), shift, 0).astype(wide)
    return total / lax.axis_size("dp")


VMEM = pl.BlockSpec(memory_space=pltpu.VMEM)
SMEM = pl.BlockSpec(memory_space=pltpu.SMEM)


def cost(rows, inner, columns):
    return pl.CostEstimate(
        flops=2 * rows * inner * columns,
        bytes_accessed=2 * (rows * inner + inner * columns + rows * columns),
        transcendentals=0,
    )


def weight_pieces(own):
    before = along_y(own, 1, 0)
    after = along_y(own, -1, 0)
    far = along_y(own, 2, 0)
    return own, after, far, before, along_y(jnp.stack((own, after, far, before)), 0, 1)


def projected(piece_refs, weight_ref, rows_ref, out_ref, first):
    size = piece_refs[0].shape[0]
    for number, ref in enumerate(piece_refs):
        rows_ref[number * size : (number + 1) * size, :] = ref[...]
    width = 256

    def tile(index, unused):
        columns = pl.ds(pl.multiple_of(index * width, width), width)
        found = dot(rows_ref[...], weight_ref[:, columns], ((1,), (0,)))
        out_ref[first : first + rows_ref.shape[0], columns] = found.astype(jnp.bfloat16)
        return unused

    lax.fori_loop(0, weight_ref.shape[1] // width, tile, 0)


def first_kernel(
    place_ref, own_ref, after_ref, far_ref, before_ref, other_ref, a_ref, b_ref, c_ref, d_ref, weight_ref, out_ref, rows_ref
):
    size = own_ref.shape[0]
    for shift, ref in enumerate((own_ref, after_ref, far_ref, before_ref)):
        weight_ref[pl.ds(pl.multiple_of(place_ref[shift], size), size), :] = ref[...]
        weight_ref[pl.ds(pl.multiple_of(place_ref[SIDE + shift], size), size), :] = other_ref[shift]
    projected((a_ref, b_ref, c_ref, d_ref), weight_ref, rows_ref, out_ref, 0)


def first_project(pieces, weights, places):
    size, width = weights[0].shape
    return pl.pallas_call(
        first_kernel,
        out_shape=[
            jax.ShapeDtypeStruct((2 * SIDE * size, width), jnp.bfloat16),
            jax.ShapeDtypeStruct((GROUP, width), jnp.bfloat16),
        ],
        in_specs=[SMEM] + [VMEM] * 9,
        out_specs=[VMEM] * 2,
        scratch_shapes=[pltpu.VMEM((GROUP, 2 * SIDE * size), jnp.bfloat16)],
        cost_estimate=cost(GROUP, 2 * SIDE * size, width),
        name="first",
    )(places * size, *weights, *pieces)


def project_kernel(*refs):
    pieces, weight_ref, out_ref, rows_ref = refs[:-3], refs[-3], refs[-2], refs[-1]
    projected(pieces, weight_ref, rows_ref, out_ref, 0)


def project(pieces, weights):
    rows = sum(piece.shape[0] for piece in pieces)
    return pl.pallas_call(
        project_kernel,
        out_shape=jax.ShapeDtypeStruct((rows, weights.shape[1]), jnp.bfloat16),
        in_specs=[VMEM] * (len(pieces) + 1),
        out_specs=VMEM,
        scratch_shapes=[pltpu.VMEM((rows, weights.shape[0]), jnp.bfloat16)],
        cost_estimate=cost(rows, *weights.shape),
        name="project",
    )(*pieces, weights)


def retention_kernel(
    rate_ref, place_ref, own_ref, sides_ref, a_ref, b_ref, c_ref, d_ref, weight_ref, cot_ref,
    out_ref, far_a_ref, far_b_ref, rows_ref, proj_ref, inner_ref, qdec_ref, kdec_ref, fwd_ref, back_ref,
):
    rate = rate_ref[0]
    dim = cot_ref.shape[1]
    steps = cot_ref.shape[0] // STEP
    blocks = STEP // (2 * HALF)
    scale = dim ** (-0.5)
    projected((a_ref, b_ref, c_ref, d_ref), weight_ref, rows_ref, proj_ref, 2 * GROUP)
    proj_ref[:GROUP, :] = own_ref[...]
    proj_ref[GROUP : 2 * GROUP, :] = sides_ref[:GROUP, :]
    proj_ref[3 * GROUP :, :] = sides_ref[GROUP:, :]

    row = lax.broadcasted_iota(jnp.int32, (STEP, STEP), 0).astype(jnp.float32)
    col = lax.broadcasted_iota(jnp.int32, (STEP, STEP), 1).astype(jnp.float32)
    spread = row - col
    inner_ref[...] = jnp.where(spread >= 0, jnp.exp(rate * jnp.maximum(spread, 0.0)), 0.0)
    at = lax.broadcasted_iota(jnp.int32, (STEP, dim), 0).astype(jnp.float32)
    qdec_ref[...] = jnp.exp(rate * (at + 1.0))
    kdec_ref[...] = jnp.exp(rate * (STEP - 1.0 - at))
    carry = jnp.exp(jnp.full((dim, dim), STEP * rate, jnp.float32))
    fwd_ref[...] = jnp.zeros_like(fwd_ref)
    back_ref[...] = jnp.zeros_like(back_ref)

    def places(index):
        found = []
        for block in range(blocks):
            for part in range(2):
                start = place_ref[part * blocks * steps + index * blocks + block]
                found.append(pl.ds(pl.multiple_of(start, HALF), HALF))
        return found

    def load(index):
        found = places(index)
        rows = jnp.concatenate([proj_ref[place, :] for place in found])
        cot = cot_ref[pl.ds(pl.multiple_of(index * STEP, STEP), STEP), :]
        keys = rows[:, dim : 2 * dim] * jnp.bfloat16(scale)
        return found, rows[:, :dim], keys, rows[:, 2 * dim :], cot

    def store(found, first, values):
        for number, place in enumerate(found):
            part = values[number * HALF : (number + 1) * HALF]
            out_ref[place, first * dim : first * dim + part.shape[1]] = part.astype(jnp.bfloat16)

    def step(index, unused):
        found, queries, keys, values, cot = load(index)
        mixed = (dot(cot, values, ((1,), (1,))) * inner_ref[...]).astype(jnp.bfloat16)
        state = fwd_ref[...]
        across = dot(cot, state.astype(jnp.bfloat16), ((1,), (0,))) * qdec_ref[...]
        grad_q = dot(mixed, keys, ((1,), (0,))) + across
        keys_w = (keys.astype(jnp.float32) * kdec_ref[...]).astype(jnp.bfloat16)
        fwd_ref[...] = state * carry + dot(values, keys_w, ((0,), (0,)))
        store(found, 0, grad_q)

        found, queries, keys, values, cot = load(steps - 1 - index)
        mixed = (dot(cot, values, ((1,), (1,))) * inner_ref[...]).astype(jnp.bfloat16)
        scores = (dot(queries, keys, ((1,), (1,))) * inner_ref[...]).astype(jnp.bfloat16)
        state = back_ref[...]
        state_bf = state.astype(jnp.bfloat16)
        grad_v = dot(scores, cot, ((0,), (0,))) + dot(keys, state_bf, ((1,), (0,))) * kdec_ref[...]
        across = dot(values, state_bf, ((1,), (1,))) * kdec_ref[...]
        grad_k = (dot(mixed, queries, ((0,), (0,))) + across) * scale
        queries_w = (queries.astype(jnp.float32) * qdec_ref[...]).astype(jnp.bfloat16)
        back_ref[...] = state * carry + dot(queries_w, cot, ((0,), (0,)))
        store(found, 1, grad_k)
        store(found, 2, grad_v)
        return unused

    lax.fori_loop(0, steps, step, 0, unroll=UNROLL)

    width = 512

    def tile(index, unused):
        columns = pl.ds(pl.multiple_of(index * width, width), width)
        total = dot(out_ref[2 * GROUP : 3 * GROUP, :], weight_ref[columns, :], ((1,), (1,)))
        far_a_ref[:, columns] = total[: GROUP // 2].astype(jnp.bfloat16)
        far_b_ref[:, columns] = total[GROUP // 2 :].astype(jnp.bfloat16)
        return unused

    lax.fori_loop(0, weight_ref.shape[0] // width, tile, 0)


def retention(rate, own, sides, far_pieces, weights, cotangent):
    length, dim = cotangent.shape
    index = lax.axis_index("sp")
    block = jnp.arange(SIDE * SIDE, dtype=jnp.int32)
    dz = (block // SIDE - index // SIDE) % SIDE
    dx = (block % SIDE - index % SIDE) % SIDE
    place = jnp.concatenate((dz * GROUP + dx * HALF, dx * GROUP + SIDE * HALF + dz * HALF))
    square = pltpu.VMEM((STEP, STEP), jnp.float32)
    wide = pltpu.VMEM((STEP, dim), jnp.float32)
    state = pltpu.VMEM((dim, dim), jnp.float32)
    return pl.pallas_call(
        retention_kernel,
        out_shape=[jax.ShapeDtypeStruct((length, 3 * dim), jnp.bfloat16)]
        + [jax.ShapeDtypeStruct((GROUP // 2, weights.shape[0]), jnp.bfloat16)] * 2,
        in_specs=[SMEM, SMEM] + [VMEM] * 8,
        out_specs=[VMEM] * 3,
        scratch_shapes=[
            pltpu.VMEM((GROUP, weights.shape[0]), jnp.bfloat16),
            pltpu.VMEM((length, 3 * dim), jnp.bfloat16),
            square, wide, wide, state, state,
        ],
        cost_estimate=cost(length, 4 * dim, 4 * dim),
        name="retention",
    )(rate, place, own, sides, *far_pieces, weights, cotangent)


def rest_kernel(grad_ref, weight_ref, *out_refs):
    low = dot(grad_ref[: 2 * GROUP, :], weight_ref[...], ((1,), (1,)))
    high = dot(grad_ref[3 * GROUP :, :], weight_ref[...], ((1,), (1,)))
    size = GROUP // 2
    for number, out_ref in enumerate(out_refs):
        source = low if number < 4 else high
        out_ref[...] = source[number % 4 * size : (number % 4 + 1) * size].astype(jnp.bfloat16)


def rest(gradients, weights):
    width = 512
    shape = jax.ShapeDtypeStruct((GROUP // 2, weights.shape[0]), jnp.bfloat16)
    return pl.pallas_call(
        rest_kernel,
        grid=(weights.shape[0] // width,),
        out_shape=[shape] * 6,
        in_specs=[
            pl.BlockSpec(gradients.shape, lambda at: (0, 0)),
            pl.BlockSpec((width, weights.shape[1]), lambda at: (at, 0)),
        ],
        out_specs=[pl.BlockSpec((GROUP // 2, width), lambda at: (0, at))] * 6,
        cost_estimate=cost(3 * GROUP, *weights.shape),
        name="rest",
    )(gradients, weights)


def collected_kernel(own_ref, after_ref, far_ref, before_ref, kept_ref, *out_refs):
    wide = jnp.float32
    for number, out_ref in enumerate((kept_ref,) + out_refs):
        rows = slice(number * HALF, (number + 1) * HALF)
        total = own_ref[rows, :].astype(wide) + after_ref[rows, :].astype(wide)
        total += far_ref[rows, :].astype(wide) + before_ref[rows, :].astype(wide)
        out_ref[...] = total.astype(out_ref.dtype)


def collected(own, after, far, before):
    rows, length = own.shape
    width = 512
    shapes = [jax.ShapeDtypeStruct((HALF, length), dtype) for dtype in (jnp.float32,) + (jnp.bfloat16,) * 3]
    return pl.pallas_call(
        collected_kernel,
        grid=(length // width,),
        out_shape=shapes,
        in_specs=[pl.BlockSpec((rows, width), lambda at: (0, at))] * 4,
        out_specs=[pl.BlockSpec((HALF, width), lambda at: (0, at))] * 4,
        cost_estimate=cost(rows, 64, length),
        name="collected",
    )(own, after, far, before)


def share_kernel(place_ref, *refs):
    pieces, grad_ref, given_ref, kept_ref, turned_ref, rows_ref = refs[:-5], *refs[-5:]
    at = pl.program_id(0)

    @pl.when(at == 0)
    def _():
        turned_ref[...] = grad_ref[...].T

    size = pieces[0].shape[0]
    for number, piece in enumerate(pieces):
        rows_ref[number * size : (number + 1) * size, :] = piece[...]
    found = dot(turned_ref[...], rows_ref[...], ((1,), (0,))).astype(jnp.bfloat16)

    @pl.when(at < SIDE)
    def _():
        given_ref[0] = found

    @pl.when(at >= SIDE)
    def _():
        kept_ref[0] = found


def share(pieces, gradients, places):
    length, width = gradients.shape
    size = pieces[0].shape[1] // (2 * SIDE)
    shape = jax.ShapeDtypeStruct((SIDE, width, size), jnp.bfloat16)
    return pl.pallas_call(
        share_kernel,
        out_shape=[shape] * 2,
        grid_spec=pltpu.PrefetchScalarGridSpec(
            num_scalar_prefetch=1,
            grid=(2 * SIDE,),
            in_specs=[
                pl.BlockSpec((piece.shape[0], size), lambda at, place: (0, place[at])) for piece in pieces
            ]
            + [pl.BlockSpec((length, width), lambda at, place: (0, 0))],
            out_specs=[
                pl.BlockSpec((1, width, size), lambda at, place: (jnp.minimum(at, SIDE - 1), 0, 0)),
                pl.BlockSpec((1, width, size), lambda at, place: (jnp.maximum(at - SIDE, 0), 0, 0)),
            ],
            scratch_shapes=[pltpu.VMEM((width, length), jnp.bfloat16), pltpu.VMEM((length, size), jnp.bfloat16)],
        ),
        cost_estimate=cost(2 * SIDE * size, length, width),
        name="share",
    )(places, *pieces, gradients)


def body(hidden_in, mix_cotangent, query_weight, key_weight, value_weight, decay_log):
    columns = query_weight.shape[1]
    index = lax.axis_index("dp")
    y, core = index // 2, index % 2
    distance = (y + jnp.arange(SIDE, dtype=jnp.int32)) % SIDE
    kept, given = distance * 2 + core, distance * 2 + 1 - core
    rows = hidden_in[0]
    a_groups = gathered(rows[:HALF], "x", "z")
    b_groups = gathered(rows[HALF:], "z", "x")
    groups = [a + b for a, b in zip(a_groups, b_groups)]
    cotangent = lax.all_to_all(mix_cotangent[0], "sp", split_axis=1, concat_axis=0, tiled=True)
    pieces = weight_pieces(jnp.concatenate((query_weight, key_weight, value_weight), axis=1))
    weights, own = first_project(groups[0], pieces, jnp.concatenate((kept, given)))
    sides = project(groups[1] + groups[3], weights)
    gradients, far_a, far_b = retention(decay_log, own, sides, groups[2], weights, cotangent)
    own_a, own_b, after_a, after_b, before_a, before_b = rest(gradients, weights)
    sum_a = reduced(own_a, after_a, far_a, before_a, "x", "z")
    sum_b = reduced(own_b, after_b, far_b, before_b, "z", "x")
    pieces = [piece for group in groups for piece in group]
    summed = weight_sum(*share(pieces, gradients, jnp.concatenate((given, kept))))
    grad_hidden = jnp.concatenate((sum_a, sum_b)).astype(jnp.bfloat16)[None]
    return (
        grad_hidden,
        summed[:columns].T,
        summed[columns : 2 * columns].T,
        summed[2 * columns :].T,
    )


def solution(mesh):
    placed = (
        P("dp", "sp", None),
        P("dp", "sp", None),
        P("dp", "sp"),
        P("dp", "sp"),
        P("dp", "sp"),
        P("sp"),
    )
    return jax.shard_map(
        body,
        mesh=mesh,
        in_specs=placed,
        out_specs=(P("dp", "sp", None), P("dp", "sp"), P("dp", "sp"), P("dp", "sp")),
        check_vma=False,
    )
```
